32 devices in a mesh: sp: 8 (over z, x), tp: 4 (over y, core).
Axes of the slice: x: 2, y: 2, z: 4, core: 2. Of those that a mesh axis runs over, the one named last changes fastest.
Arguments:
- tokens: bfloat16 [2048, 3072], P('sp', 'tp'), may hold values from -6 to 6
- norm_gain: float32 [3072], replicated, may hold values from 0.1 to 1.9
- state_in_weight: bfloat16 [3072, 1024], P('sp', 'tp'), may hold values from -0.109375 to 0.109375
- pool_in_weight: bfloat16 [3072, 1024], P('sp', 'tp'), may hold values from -0.109375 to 0.109375
- rate_real: float32 [64, 64], replicated, may hold values from -1.5 to -0.5
- rate_imag: float32 [64, 64], replicated, may hold values from 0 to 200
- log_step: float32 [64], replicated, may hold values from -2 to 0.7
- input_real: float32 [64, 64, 16], replicated, may hold values from -1 to 1
- input_imag: float32 [64, 64, 16], replicated, may hold values from -1 to 1
- output_real: float32 [64, 16, 64], replicated, may hold values from -64 to 64
- output_imag: float32 [64, 16, 64], replicated, may hold values from -64 to 64
- skip_gain: float32 [1024], replicated, may hold values from -3 to 3
- pool_weight: bfloat16 [16, 64, 64], replicated, may hold values from -0.75 to 0.75
- pool_gain: float32 [1024], replicated, may hold values from 0.1 to 1.9
- state_out_weight: bfloat16 [1024, 3072], P('sp', 'tp'), may hold values from -0.125 to 0.125
- pool_out_weight: bfloat16 [1024, 3072], P('sp', 'tp'), may hold values from -0.125 to 0.125
Outputs:
- mixer_output: bfloat16 [2048, 3072], P('sp', 'tp')
The draws below stay inside these ranges and needn't reach their ends.
All inputs are finite; a program needn't handle non-finite values.
Results may differ from the reference program's by a relative error of at most 0.0065.
Values may be sent and summed in bfloat16 or wider, within the bound.
A program may use at most 64 MiB of HBM per device.

```python
import jax
import jax.numpy as jnp
from jax import lax

D = 3072
SSM_GROUP = 16
SSM_GROUPS = 64
SSM_STATE = 64
POOL_GROUP = 64
POOL_GROUPS = 16
TOKENS = 2048
D_SSM = 1024
D_POOL = 1024


def level_of(key, dims, cuts, smallest, largest):
    gain, own = 1.0, jax.random.fold_in(key, 6)
    for axis_at, shards_of in cuts:
        draws = jnp.exp(jax.random.uniform(jax.random.fold_in(own, axis_at), (shards_of,), jnp.float32, smallest / len(cuts), largest / len(cuts)))
        gain = gain * jnp.repeat(draws, dims[axis_at] // shards_of).reshape([-1 if axis == axis_at else 1 for axis in range(len(dims))])
    return gain


def normal_values(rng, extent, scale, limit, split=(), held_as=jnp.bfloat16):
    array = scale * jax.random.normal(rng, extent, jnp.float32)
    if split:
        array = array * level_of(rng, extent, split, -0.22, 0.18)
    return jnp.clip(array, -limit, limit).astype(held_as)


def setup_inputs(seed: int = 0) -> dict:
    streams_of = jax.random.split(jax.random.key(seed), 17)
    return {
        "tokens": normal_values(streams_of[0], (TOKENS, D), 1.0, 6.0, ((0, 8), (1, 4))),
        "norm_gain": jnp.clip(1.0 + 0.18 * jax.random.normal(streams_of[1], (D,), jnp.float32), 0.1, 1.9),
        "state_in_weight": normal_values(streams_of[2], (D, D_SSM), D ** -0.5, 0.109375, ((0, 8), (1, 4))),
        "pool_in_weight": normal_values(streams_of[3], (D, D_POOL), D ** -0.5, 0.109375, ((0, 8), (1, 4))),
        "rate_real": jnp.clip(jax.random.uniform(streams_of[4], (SSM_GROUPS, SSM_STATE), jnp.float32, -1.5, -0.5), -1.5, -0.5),
        "rate_imag": jnp.clip(jax.random.uniform(streams_of[5], (SSM_GROUPS, SSM_STATE), jnp.float32, 0.0, 200.0), 0.0, 200.0),
        "log_step": jnp.clip(jax.random.uniform(streams_of[6], (SSM_GROUPS,), jnp.float32, -2.0, 0.7), -2.0, 0.7),
        "input_real": normal_values(streams_of[7], (SSM_GROUPS, SSM_STATE, SSM_GROUP), (2 * SSM_GROUP) ** -0.5, 1.0, (), jnp.float32),
        "input_imag": normal_values(streams_of[8], (SSM_GROUPS, SSM_STATE, SSM_GROUP), (2 * SSM_GROUP) ** -0.5, 1.0, (), jnp.float32),
        "output_real": normal_values(streams_of[9], (SSM_GROUPS, SSM_GROUP, SSM_STATE), (TOKENS // 256 + 2), 64.0, (), jnp.float32),
        "output_imag": normal_values(streams_of[10], (SSM_GROUPS, SSM_GROUP, SSM_STATE), (TOKENS // 256 + 2), 64.0, (), jnp.float32),
        "skip_gain": normal_values(streams_of[11], (D_SSM,), 0.5, 3.0, (), jnp.float32),
        "pool_weight": normal_values(streams_of[12], (POOL_GROUPS, POOL_GROUP, POOL_GROUP), POOL_GROUP ** -0.5, 0.75),
        "pool_gain": jnp.clip(1.0 + 0.18 * jax.random.normal(streams_of[13], (D_POOL,), jnp.float32), 0.1, 1.9),
        "state_out_weight": normal_values(streams_of[14], (D_SSM, D), (D_SSM + D_POOL) ** -0.5, 0.125, ((0, 8), (1, 4))),
        "pool_out_weight": normal_values(streams_of[15], (D_POOL, D), (D_SSM + D_POOL) ** -0.5, 0.125, ((0, 8), (1, 4))),
    }


epsilon = 1e-06
highest = lax.Precision.HIGHEST

def discretize(rate_real, rate_imag, log_step, length):
    step_size = jnp.exp(log_step)[:, None] / length
    exponent = rate_real * step_size
    angle = rate_imag * step_size
    magnitude = jnp.exp(exponent)
    decay_real = magnitude * jnp.cos(angle)
    decay_imag = magnitude * jnp.sin(angle)
    less_one = jnp.expm1(exponent) * jnp.cos(angle) - 2.0 * jnp.square(jnp.sin(0.5 * angle))
    denominator = rate_real * rate_real + rate_imag * rate_imag
    factor_real = (less_one * rate_real + decay_imag * rate_imag) / denominator
    factor_imag = (decay_imag * rate_real - less_one * rate_imag) / denominator
    return (exponent, angle, decay_real, decay_imag, factor_real, factor_imag)

def drive_terms(signal, factor_real, factor_imag, input_real, input_imag):
    drive_real = factor_real[..., None] * input_real - factor_imag[..., None] * input_imag
    drive_imag = factor_real[..., None] * input_imag + factor_imag[..., None] * input_real
    push_real = jnp.einsum('tgc,gnc->tgn', signal, drive_real, precision=highest)
    push_imag = jnp.einsum('tgc,gnc->tgn', signal, drive_imag, precision=highest)
    return (push_real, push_imag)

def readout(states_real, states_imag, output_real, output_imag, signal, skip_gain):
    row_count = states_real.shape[0]
    readout_sum = jnp.einsum('tgn,gcn->tgc', states_real, output_real, precision=highest)
    readout_sum = readout_sum - jnp.einsum('tgn,gcn->tgc', states_imag, output_imag, precision=highest)
    readout_sum = readout_sum.reshape(row_count, -1) + skip_gain * signal.reshape(row_count, -1)
    return jax.nn.gelu(readout_sum).astype(jnp.bfloat16)

def pool_mixer(pool_in, pool_weight, pool_gain):
    row_count = pool_in.shape[0]
    signal = pool_in.astype(jnp.float32).reshape(row_count, POOL_GROUPS, POOL_GROUP)
    running = jnp.cumsum(signal, axis=0)
    padded = jnp.pad(running, ((16, 0), (0, 0), (0, 0)))
    positions = jnp.arange(1, row_count + 1)
    window_means = []
    for group_index in range(POOL_GROUPS):
        window = 2 ** (group_index % 4 + 1)
        lagged = padded[16 - window:16 - window + row_count, group_index]
        divisor = jnp.minimum(positions, window).astype(jnp.float32)[:, None]
        window_means.append((running[:, group_index] - lagged) / divisor)
    pooled = jnp.stack(window_means, axis=1) - signal
    projected = jnp.einsum('tgc,gcd->tgd', pooled, pool_weight.astype(jnp.float32), precision=highest)
    return (projected.reshape(row_count, -1) * pool_gain).astype(jnp.bfloat16)

def reference(tokens, norm_gain, state_in_weight, pool_in_weight, rate_real, rate_imag, log_step, input_real, input_imag, output_real, output_imag, skip_gain, pool_weight, pool_gain, state_out_weight, pool_out_weight):
    features = tokens.astype(jnp.float32)
    inverse = lax.rsqrt(lax.optimization_barrier(jnp.sum(features * features, axis=1)) / D + epsilon)[:, None]
    scaled = (features * norm_gain).astype(jnp.bfloat16)
    state_in = (jnp.dot(scaled, state_in_weight, preferred_element_type=jnp.float32) * inverse).astype(jnp.bfloat16)
    pool_in = (jnp.dot(scaled, pool_in_weight, preferred_element_type=jnp.float32) * inverse).astype(jnp.bfloat16)
    signal = state_in.astype(jnp.float32).reshape(TOKENS, SSM_GROUPS, SSM_GROUP)
    exponent, angle, decay_real, decay_imag, factor_real, factor_imag = discretize(rate_real, rate_imag, log_step, TOKENS)
    push_real, push_imag = drive_terms(signal, factor_real, factor_imag, input_real, input_imag)

    def advance(carry, pushes):
        state_real, state_imag = carry
        next_real = decay_real * state_real - decay_imag * state_imag + pushes[0]
        next_imag = decay_real * state_imag + decay_imag * state_real + pushes[1]
        return ((next_real, next_imag), (next_real, next_imag))
    zero_state = jnp.zeros((SSM_GROUPS, SSM_STATE), jnp.float32)
    _, (states_real, states_imag) = lax.scan(advance, (zero_state, zero_state), (push_real, push_imag))
    state_out = readout(states_real, states_imag, output_real, output_imag, signal, skip_gain)
    pool_out = pool_mixer(pool_in, pool_weight, pool_gain)
    combined = jnp.dot(state_out, state_out_weight, preferred_element_type=jnp.float32)
    combined = combined + jnp.dot(pool_out, pool_out_weight, preferred_element_type=jnp.float32)
    return combined.astype(jnp.bfloat16)
```

```python
import functools

import jax
import jax.numpy as jnp
from jax import lax
from jax.experimental import pallas as pl
from jax.experimental.pallas import tpu as pltpu
from jax.sharding import PartitionSpec as P

SSM_GROUP = 16
POOL_GROUP = 64
CHUNKS = 8
PIECES = 2

epsilon = 1e-06
window_reach = 16
f32, bf16 = jnp.float32, jnp.bfloat16
MESH = pl.DeviceIdType.MESH


def discretize(rate_real, rate_imag, log_step, length):
    step_size = jnp.exp(log_step)[:, None] / length
    exponent = rate_real * step_size
    angle = rate_imag * step_size
    magnitude = jnp.exp(exponent)
    decay_real = magnitude * jnp.cos(angle)
    decay_imag = magnitude * jnp.sin(angle)
    less_one = jnp.expm1(exponent) * jnp.cos(angle) - 2.0 * jnp.square(jnp.sin(0.5 * angle))
    denominator = rate_real * rate_real + rate_imag * rate_imag
    factor_real = (less_one * rate_real + decay_imag * rate_imag) / denominator
    factor_imag = (decay_imag * rate_real - less_one * rate_imag) / denominator
    return decay_real, decay_imag, factor_real, factor_imag


def iota(shape, axis):
    return lax.broadcasted_iota(jnp.int32, shape, axis)


def dot(a, b):
    return jnp.dot(a, b, preferred_element_type=f32)


def dot_nt(a, b):
    return lax.dot_general(a, b, (((1,), (1,)), ((), ())), preferred_element_type=f32)


def split(a):
    high = a.astype(bf16)
    return high, (a - high.astype(f32)).astype(bf16)


def cmul(ar, ai, br, bi):
    return ar * br - ai * bi, ar * bi + ai * br


def kernel(
    n_sp, n_tp, n_x, states,
    tok_ref, gain_ref, wsi_ref, wpi_ref, dec_ref, drive_ref, read_ref, skip_ref, pw_ref, pg_ref,
    wso_ref, wpo_ref,
    out_ref,
    tok_full, wsi, wpi, wso, wpo, scaled, dmat, rmat, pmat, push, ext, halo, ends, act,
    mine_s, mine_p, halo_out,
    own_sem, ring_send, ring_recv, tok_send, tok_recv, act_send, act_recv, halo_sem, end_send, end_recv,
):
    me, tp = lax.axis_index("sp"), lax.axis_index("tp")
    n_z = n_sp // n_x
    rows = tok_ref.shape[0]
    features = tok_ref.shape[1]
    width = wsi_ref.shape[1]
    pool_width = wpi_ref.shape[1]
    columns = dec_ref.shape[1]
    span = rows // CHUNKS

    def place(p):
        x, r = p // n_z, p % n_z
        return (r + (x % 2) * (n_z - 1 - 2 * r)) * n_x + x

    my_x, my_z = me % n_x, me // n_x
    at = my_x * n_z + my_z + (my_x % 2) * (n_z - 1 - 2 * my_z)

    barrier = pltpu.get_barrier_semaphore()
    for k in range(1, n_sp):
        pl.semaphore_signal(barrier, inc=1, device_id=((me + k) % n_sp, tp), device_id_type=MESH)
    for k in range(1, n_tp):
        pl.semaphore_signal(barrier, inc=1, device_id=(me, (tp + k) % n_tp), device_id_type=MESH)

    fulls = ((wsi_ref, wsi), (wpi_ref, wpi), (wso_ref, wso), (wpo_ref, wpo))
    owns = []
    for a, (own, full) in enumerate(fulls):
        count = own.shape[0]
        owns.append(
            pltpu.make_async_copy(
                own, full.at[pl.ds(pl.multiple_of(me * count, count), count)], own_sem.at[a]
            )
        )
    owns.append(pltpu.make_async_copy(tok_ref, tok_full.at[tp], own_sem.at[4]))
    for c in owns:
        c.start()
    pl.semaphore_wait(barrier, n_sp - 1 + n_tp - 1)

    def part(a, s, h):
        own, full = fulls[a]
        count = own.shape[0]
        size = count // PIECES
        way = 1 if a % 2 == 0 else -1
        owner = place((at - way * s + n_sp) % n_sp)
        there = full.at[pl.ds(pl.multiple_of(owner * count + h * size, size), size)]
        source = own.at[pl.ds(h * size, size)] if s == 0 else there
        return source, there, (place((at + way + n_sp) % n_sp), tp)

    def sender(a, s, h):
        source, there, target = part(a, s, h)
        return pltpu.make_async_remote_copy(
            source, there, ring_send.at[a, s, h], ring_recv.at[a, s, h],
            device_id=target, device_id_type=MESH,
        )

    def arrive(a, s, h):
        _, there, target = part(a, s + 1, h)
        pltpu.make_async_remote_copy(
            there, there, ring_send.at[a, s, h], ring_recv.at[a, s, h],
            device_id=target, device_id_type=MESH,
        ).wait_recv()

    last = n_sp - 2

    def ring(phase, s):
        for h in range(PIECES):
            for a in (2 * phase, 2 * phase + 1):
                arrive(a, s, h)
                if s < last:
                    sender(a, s + 1, h).start()
                    if s + 1 == last and phase == 0:
                        sender(a + 2, 0, h).start()

    def token_copy(k):
        return pltpu.make_async_remote_copy(
            tok_ref, tok_full.at[tp], tok_send.at[k - 1], tok_recv.at[k - 1],
            device_id=(me, (tp + k) % n_tp), device_id_type=MESH,
        )

    for h in range(PIECES):
        for a in (0, 1):
            sender(a, 0, h).start()
    for k in range(1, n_tp):
        token_copy(k).start()

    def build_drive(i):
        spread = (iota((width, SSM_GROUP), 0) % SSM_GROUP == iota((width, SSM_GROUP), 1)).astype(bf16)
        same = iota((width, columns), 0) // SSM_GROUP == iota((width, columns), 1) // states
        for j, piece in enumerate(split(drive_ref[i])):
            dmat[i, j] = jnp.where(same, dot_nt(spread, piece), 0.0).astype(bf16)

    def build_read(i):
        spread = (iota((columns, states), 0) % states == iota((columns, states), 1)).astype(bf16)
        same = iota((columns, width), 0) // states == iota((columns, width), 1) // SSM_GROUP
        for j, piece in enumerate(split(read_ref[i])):
            rmat[i, j] = jnp.where(same, dot_nt(spread, piece), 0.0).astype(bf16)

    def build_pool():
        spread = (
            iota((POOL_GROUP, pool_width), 0) == iota((POOL_GROUP, pool_width), 1) % POOL_GROUP
        ).astype(bf16)
        same = iota((pool_width, pool_width), 0) // POOL_GROUP == iota((pool_width, pool_width), 1) // POOL_GROUP
        pmat[...] = jnp.where(same, dot(pw_ref[...], spread), 0.0).astype(bf16)

    first = [
        lambda: build_drive(0), lambda: build_drive(1), lambda: build_read(0),
        lambda: build_read(1), build_pool,
    ]
    squares = []

    def take(t):
        block = tok_full[t].astype(f32)
        squares.append(jnp.sum(block * block, axis=1, keepdims=True))
        cut = slice(t * features, (t + 1) * features)
        scaled[:, cut] = (block * gain_ref[:, cut]).astype(bf16)

    def tokens_in():
        owns[4].wait()
        for k in range(1, n_tp):
            pltpu.make_async_remote_copy(
                tok_ref, tok_full.at[(tp - k + n_tp) % n_tp], tok_send.at[k - 1], tok_recv.at[k - 1],
                device_id=(me, (tp + k) % n_tp), device_id_type=MESH,
            ).wait_recv()

    for s in range(n_sp - 1):
        if s < len(first):
            first[s]()
        ring(0, s)
    for rest in first[n_sp - 1 :]:
        rest()
    tokens_in()
    for t in range(n_tp):
        take(t)
    owns[0].wait()
    owns[1].wait()
    inverse = lax.rsqrt(sum(squares) / (features * n_tp) + epsilon)
    pool_in = (dot(scaled[...], wpi[...]) * inverse).astype(bf16)
    ext[window_reach:] = pool_in
    halo_out[...] = pool_in[rows - window_reach :]
    state_in = (dot(scaled[...], wsi[...]) * inverse).astype(bf16)
    halo_copy = pltpu.make_async_remote_copy(
        halo_out, halo, halo_sem.at[0], halo_sem.at[1],
        device_id=((me + 1) % n_sp, tp), device_id_type=MESH,
    )
    halo_copy.start()
    done = [0]

    def step():
        if done[0] < n_sp - 1:
            ring(1, done[0])
            done[0] += 1

    step()
    shuffle = (
        iota((rows, rows), 1)
        == (iota((rows, rows), 0) % CHUNKS) * span + iota((rows, rows), 0) // CHUNKS
    ).astype(bf16)
    signal = dot(shuffle, state_in).astype(bf16)
    for i in range(2):
        push[i] = dot(signal, dmat[i, 0]) + dot(signal, dmat[i, 1])
    step()
    decay_real = jnp.broadcast_to(dec_ref[0:1, :], (CHUNKS, columns))
    decay_imag = jnp.broadcast_to(dec_ref[1:2, :], (CHUNKS, columns))

    def advance(p, carry):
        cut = pl.ds(pl.multiple_of(p * CHUNKS, CHUNKS), CHUNKS)
        real, imag = cmul(decay_real, decay_imag, *carry)
        real, imag = real + push[0, cut, :], imag + push[1, cut, :]
        push[0, cut, :] = real
        push[1, cut, :] = imag
        return real, imag

    zero = jnp.zeros((CHUNKS, columns), f32)
    end_real, end_imag = lax.fori_loop(0, span, advance, (zero, zero))

    def power(real, imag, count):
        out = None
        while count:
            if count % 2:
                out = (real, imag) if out is None else cmul(*out, real, imag)
            real, imag = cmul(real, imag, real, imag)
            count //= 2
        return out

    chunk_decay = power(dec_ref[0:1, :], dec_ref[1:2, :], span)
    block_decay = power(*chunk_decay, CHUNKS)
    row_zero = jnp.zeros((1, columns), f32)
    total = (row_zero, row_zero)
    for j in range(CHUNKS):
        moved = cmul(*chunk_decay, *total)
        total = (moved[0] + end_real[j : j + 1], moved[1] + end_imag[j : j + 1])
    which = iota((CHUNKS, columns), 0)
    ends[me] = jnp.where(which == 0, total[0], jnp.where(which == 1, total[1], 0.0))
    step()

    def end_copy(k):
        return pltpu.make_async_remote_copy(
            ends.at[me], ends.at[me], end_send.at[k - 1], end_recv.at[k - 1],
            device_id=((me + k) % n_sp, tp), device_id_type=MESH,
        )

    for k in range(1, n_sp):
        end_copy(k).start()

    halo_copy.wait_recv()
    ext[:window_reach] = jnp.where(me == 0, jnp.zeros_like(halo), halo[...])
    group = tp * (pool_width // POOL_GROUP) + iota((rows, pool_width), 1) // POOL_GROUP
    window = jnp.left_shift(jnp.ones_like(group), group % 4 + 1)
    targets = iota((rows, rows + window_reach), 0) + window_reach
    sources = iota((rows, rows + window_reach), 1)
    whole = ext[...]
    sums = jnp.zeros((rows, pool_width), f32)
    for power_index in range(1, 5):
        reach = 2**power_index
        band = ((sources <= targets) & (sources > targets - reach)).astype(bf16)
        sums = jnp.where(window == reach, dot(band, whole), sums)
    position = me * rows + iota((rows, pool_width), 0)
    divisor = jnp.minimum(position + 1, window).astype(f32)
    pooled = sums / divisor - ext[window_reach:].astype(f32)
    pooled_high, pooled_low = split(pooled)
    projected = dot(pooled_high, pmat[...]) + dot(pooled_low, pmat[...])
    mine_p[...] = (projected * pg_ref[...]).astype(bf16)
    step()

    def act_copy(which, k, source):
        mine = mine_s if which == 0 else mine_p
        return pltpu.make_async_remote_copy(
            mine, act.at[which, source], act_send.at[which, k - 1], act_recv.at[which, k - 1],
            device_id=(me, (tp + k) % n_tp), device_id_type=MESH,
        )

    for k in range(1, n_tp):
        act_copy(1, k, tp).start()
    act[1, tp] = mine_p[...]

    for k in range(1, n_sp):
        there = ends.at[(me - k + n_sp) % n_sp]
        pltpu.make_async_remote_copy(
            there, there, end_send.at[k - 1], end_recv.at[k - 1],
            device_id=((me + k) % n_sp, tp), device_id_type=MESH,
        ).wait_recv()
    total = (row_zero, row_zero)
    for s in range(n_sp - 1):
        moved = cmul(*block_decay, *total)
        use = s < me
        total = (
            jnp.where(use, moved[0] + ends[s, 0:1, :], total[0]),
            jnp.where(use, moved[1] + ends[s, 1:2, :], total[1]),
        )
    begin_real, begin_imag = zero, zero
    for j in range(CHUNKS):
        begin_real = jnp.where(which == j, total[0], begin_real)
        begin_imag = jnp.where(which == j, total[1], begin_imag)
        moved = cmul(*chunk_decay, *total)
        total = (moved[0] + end_real[j : j + 1], moved[1] + end_imag[j : j + 1])

    def add_carry(p, carry):
        cut = pl.ds(pl.multiple_of(p * CHUNKS, CHUNKS), CHUNKS)
        real, imag = cmul(decay_real, decay_imag, *carry)
        push[0, cut, :] = push[0, cut, :] + real
        push[1, cut, :] = push[1, cut, :] + imag
        return real, imag

    lax.fori_loop(0, span, add_carry, (begin_real, begin_imag))
    step()
    real_high, real_low = split(push[0])
    imag_high, imag_low = split(push[1])
    readout = dot(real_high, rmat[0, 0]) + dot(real_high, rmat[0, 1]) + dot(real_low, rmat[0, 0])
    readout -= dot(imag_high, rmat[1, 0]) + dot(imag_high, rmat[1, 1]) + dot(imag_low, rmat[1, 0])
    readout += skip_ref[...] * signal.astype(f32)
    shuffled = jax.nn.gelu(readout).astype(bf16)
    restore = (
        iota((rows, rows), 0)
        == (iota((rows, rows), 1) % CHUNKS) * span + iota((rows, rows), 1) // CHUNKS
    ).astype(bf16)
    mine_s[...] = dot(restore, shuffled).astype(bf16)
    step()
    for k in range(1, n_tp):
        act_copy(0, k, tp).start()
    act[0, tp] = mine_s[...]
    while done[0] < n_sp - 1:
        step()
    for which in (1, 0):
        for k in range(1, n_tp):
            act_copy(which, k, (tp - k + n_tp) % n_tp).wait_recv()
    owns[2].wait()
    owns[3].wait()
    result = None
    for t in range(n_tp):
        for which, full, size in ((1, wpo, pool_width), (0, wso, width)):
            term = dot(act[which, t], full[t * size : (t + 1) * size, :])
            result = term if result is None else result + term
    out_ref[...] = result.astype(bf16)

    for a in range(4):
        for s in range(n_sp - 1):
            for h in range(PIECES):
                sender(a, s, h).wait_send()
    for k in range(1, n_tp):
        token_copy(k).wait_send()
        act_copy(0, k, tp).wait_send()
        act_copy(1, k, tp).wait_send()
    halo_copy.wait_send()
    for k in range(1, n_sp):
        end_copy(k).wait_send()


def body(
    n_sp, n_tp, n_x,
    tokens, norm_gain, state_in_weight, pool_in_weight, rate_real, rate_imag, log_step,
    input_real, input_imag, output_real, output_imag, skip_gain, pool_weight, pool_gain,
    state_out_weight, pool_out_weight,
):
    rows, features = tokens.shape
    in_rows, width = state_in_weight.shape
    pool_width = pool_in_weight.shape[1]
    out_rows, out_columns = state_out_weight.shape
    groups = width // SSM_GROUP
    states = rate_real.shape[1]
    columns = groups * states
    pool_groups = pool_width // POOL_GROUP
    tp = lax.axis_index("tp")

    def mine(a, count):
        return lax.dynamic_slice_in_dim(a, tp * count, count, 0)

    decay_real, decay_imag, factor_real, factor_imag = discretize(
        mine(rate_real, groups), mine(rate_imag, groups), mine(log_step, groups), rows * n_sp
    )
    local_real, local_imag = mine(input_real, groups), mine(input_imag, groups)
    drive = jnp.stack(
        [
            factor_real[..., None] * local_real - factor_imag[..., None] * local_imag,
            factor_real[..., None] * local_imag + factor_imag[..., None] * local_real,
        ]
    ).reshape(2, columns, SSM_GROUP)
    read = jnp.stack([mine(output_real, groups), mine(output_imag, groups)]).reshape(2, width, states)
    decay = jnp.stack([decay_real, decay_imag]).reshape(2, columns)
    pool_matrix = mine(pool_weight, pool_groups).reshape(pool_width, POOL_GROUP)
    vmem = pl.BlockSpec(memory_space=pltpu.VMEM)
    dma = pltpu.SemaphoreType.DMA
    return pl.pallas_call(
        functools.partial(kernel, n_sp, n_tp, n_x, states),
        out_shape=jax.ShapeDtypeStruct((rows, out_columns), bf16),
        in_specs=[vmem] * 12,
        out_specs=vmem,
        scratch_shapes=[
            pltpu.VMEM((n_tp, rows, features), bf16),
            pltpu.VMEM((n_sp * in_rows, width), bf16),
            pltpu.VMEM((n_sp * in_rows, pool_width), bf16),
            pltpu.VMEM((n_sp * out_rows, out_columns), bf16),
            pltpu.VMEM((n_sp * out_rows, out_columns), bf16),
            pltpu.VMEM((rows, features * n_tp), bf16),
            pltpu.VMEM((2, 2, width, columns), bf16),
            pltpu.VMEM((2, 2, columns, width), bf16),
            pltpu.VMEM((pool_width, pool_width), bf16),
            pltpu.VMEM((2, rows, columns), f32),
            pltpu.VMEM((rows + window_reach, pool_width), bf16),
            pltpu.VMEM((window_reach, pool_width), bf16),
            pltpu.VMEM((n_sp, CHUNKS, columns), f32),
            pltpu.VMEM((2, n_tp, rows, width), bf16),
            pltpu.VMEM((rows, width), bf16),
            pltpu.VMEM((rows, pool_width), bf16),
            pltpu.VMEM((window_reach, pool_width), bf16),
            dma((5,)),
            dma((4, n_sp - 1, PIECES)),
            dma((4, n_sp - 1, PIECES)),
            dma((n_tp - 1,)),
            dma((n_tp - 1,)),
            dma((2, n_tp - 1)),
            dma((2, n_tp - 1)),
            dma((2,)),
            dma((n_sp - 1,)),
            dma((n_sp - 1,)),
        ],
        compiler_params=pltpu.CompilerParams(
            collective_id=0, has_side_effects=True, vmem_limit_bytes=60 * 2**20
        ),
    )(
        tokens, norm_gain[None], state_in_weight, pool_in_weight, decay, drive, read,
        mine(skip_gain, width)[None], pool_matrix, mine(pool_gain, pool_width)[None],
        state_out_weight, pool_out_weight,
    )


def solution(mesh):
    n_sp, n_tp = mesh.shape["sp"], mesh.shape["tp"]
    n_x = 2 ** ((n_sp.bit_length() - 1) // 2)
    both, whole = P("sp", "tp"), P()
    return jax.shard_map(
        functools.partial(body, n_sp, n_tp, n_x),
        mesh=mesh,
        in_specs=(both, whole, both, both) + (whole,) * 10 + (both, both),
        out_specs=both,
        check_vma=False,
    )
```

```python
import functools

import jax
import jax.numpy as jnp
from jax import lax
from jax.experimental import pallas as pl
from jax.experimental.pallas import tpu as pltpu
from jax.sharding import PartitionSpec as P

SSM_GROUP = 16
POOL_GROUP = 64
CHUNKS = 8
PIECES = 2

epsilon = 1e-06
window_reach = 16
f32, bf16 = jnp.float32, jnp.bfloat16
MESH = pl.DeviceIdType.MESH


def discretize(rate_real, rate_imag, log_step, length):
    step_size = jnp.exp(log_step)[:, None] / length
    exponent = rate_real * step_size
    angle = rate_imag * step_size
    magnitude = jnp.exp(exponent)
    decay_real = magnitude * jnp.cos(angle)
    decay_imag = magnitude * jnp.sin(angle)
    less_one = jnp.expm1(exponent) * jnp.cos(angle) - 2.0 * jnp.square(jnp.sin(0.5 * angle))
    denominator = rate_real * rate_real + rate_imag * rate_imag
    factor_real = (less_one * rate_real + decay_imag * rate_imag) / denominator
    factor_imag = (decay_imag * rate_real - less_one * rate_imag) / denominator
    return decay_real, decay_imag, factor_real, factor_imag


def iota(shape, axis):
    return lax.broadcasted_iota(jnp.int32, shape, axis)


def dot(a, b):
    return jnp.dot(a, b, preferred_element_type=f32)


def dot_nt(a, b):
    return lax.dot_general(a, b, (((1,), (1,)), ((), ())), preferred_element_type=f32)


def split(a):
    high = a.astype(bf16)
    return high, (a - high.astype(f32)).astype(bf16)


def cmul(ar, ai, br, bi):
    return ar * br - ai * bi, ar * bi + ai * br


def kernel(
    n_sp, n_tp, n_x, states,
    tok_ref, gain_ref, wsi_ref, wpi_ref, rr_ref, ri_ref, step_ref, inr_ref, ini_ref, outr_ref,
    outi_ref, skip_ref, pw_ref, pg_ref, wso_ref, wpo_ref,
    out_ref,
    tok_full, wsi, wpi, wso, wpo, scaled, dmat, rmat, pmat, push, ext, halo, ends, act,
    mine_s, mine_p, halo_out, rates, matrices, pool_own, dec_ref,
    own_sem, ring_send, ring_recv, tok_send, tok_recv, act_send, act_recv, halo_sem, end_send, end_recv,
):
    me, tp = lax.axis_index("sp"), lax.axis_index("tp")
    n_z = n_sp // n_x
    rows = tok_ref.shape[0]
    features = tok_ref.shape[1]
    width = wsi_ref.shape[1]
    pool_width = wpi_ref.shape[1]
    groups = width // SSM_GROUP
    columns = groups * states
    pool_groups = pool_width // POOL_GROUP
    span = rows // CHUNKS

    def place(p):
        x, r = p // n_z, p % n_z
        return (r + (x % 2) * (n_z - 1 - 2 * r)) * n_x + x

    my_x, my_z = me % n_x, me // n_x
    at = my_x * n_z + my_z + (my_x % 2) * (n_z - 1 - 2 * my_z)

    barrier = pltpu.get_barrier_semaphore()
    for k in range(1, n_sp):
        pl.semaphore_signal(barrier, inc=1, device_id=((me + k) % n_sp, tp), device_id_type=MESH)
    for k in range(1, n_tp):
        pl.semaphore_signal(barrier, inc=1, device_id=(me, (tp + k) % n_tp), device_id_type=MESH)

    fulls = ((wsi_ref, wsi), (wpi_ref, wpi), (wso_ref, wso), (wpo_ref, wpo))
    owns = []
    for a, (own, full) in enumerate(fulls):
        count = own.shape[0]
        owns.append(
            pltpu.make_async_copy(
                own, full.at[pl.ds(pl.multiple_of(me * count, count), count)], own_sem.at[a]
            )
        )
    owns.append(pltpu.make_async_copy(tok_ref, tok_full.at[tp], own_sem.at[4]))
    def heads(ref, count):
        return ref.at[pl.ds(pl.multiple_of(tp * count, count), count)]

    loads = [
        pltpu.make_async_copy(heads(ref, groups), there, own_sem.at[5 + k])
        for k, (ref, there) in enumerate(
            (
                (rr_ref, rates.at[0]), (ri_ref, rates.at[1]), (inr_ref, matrices.at[0]),
                (ini_ref, matrices.at[1]), (outr_ref, matrices.at[2]), (outi_ref, matrices.at[3]),
            )
        )
    ]
    loads.append(pltpu.make_async_copy(heads(pw_ref, pool_groups), pool_own, own_sem.at[11]))
    for c in owns + loads:
        c.start()
    pl.semaphore_wait(barrier, n_sp - 1 + n_tp - 1)

    def part(a, s, h):
        own, full = fulls[a]
        count = own.shape[0]
        size = count // PIECES
        way = 1 if a % 2 == 0 else -1
        owner = place((at - way * s + n_sp) % n_sp)
        there = full.at[pl.ds(pl.multiple_of(owner * count + h * size, size), size)]
        source = own.at[pl.ds(h * size, size)] if s == 0 else there
        return source, there, (place((at + way + n_sp) % n_sp), tp)

    def sender(a, s, h):
        source, there, target = part(a, s, h)
        return pltpu.make_async_remote_copy(
            source, there, ring_send.at[a, s, h], ring_recv.at[a, s, h],
            device_id=target, device_id_type=MESH,
        )

    def arrive(a, s, h):
        _, there, target = part(a, s + 1, h)
        pltpu.make_async_remote_copy(
            there, there, ring_send.at[a, s, h], ring_recv.at[a, s, h],
            device_id=target, device_id_type=MESH,
        ).wait_recv()

    last = n_sp - 2

    def ring(phase, s, h):
        for a in (2 * phase, 2 * phase + 1):
            arrive(a, s, h)
            if s < last:
                sender(a, s + 1, h).start()
                if s + 1 == last and phase == 0:
                    sender(a + 2, 0, h).start()

    turns = [(phase, s, h) for phase in range(2) for s in range(n_sp - 1) for h in range(PIECES)]
    turn = [0]

    def step(stop=len(turns)):
        if turn[0] < stop:
            ring(*turns[turn[0]])
            turn[0] += 1

    def token_copy(k):
        return pltpu.make_async_remote_copy(
            tok_ref, tok_full.at[tp], tok_send.at[k - 1], tok_recv.at[k - 1],
            device_id=(me, (tp + k) % n_tp), device_id_type=MESH,
        )

    for h in range(PIECES):
        for a in (0, 1):
            sender(a, 0, h).start()
    for k in range(1, n_tp):
        token_copy(k).start()

    tile = iota((states, columns), 0) == iota((states, columns), 1) % states
    tile_exact, tile_half = tile.astype(f32), tile.astype(bf16)

    def exactly(a, b):
        return jnp.dot(a, b, precision=lax.Precision.HIGHEST, preferred_element_type=f32)

    factors = []

    def build_decay():
        for c in loads:
            c.wait()
        own_head = iota((groups, columns), 0) == iota((groups, columns), 1) // states

        def flat(a):
            return jnp.sum(jnp.where(own_head, exactly(a, tile_exact), 0.0), axis=0, keepdims=True)

        rate_real, rate_imag = flat(rates[0]), flat(rates[1])
        all_groups = step_ref.shape[1]
        head = iota((all_groups, columns), 0) == tp * groups + iota((all_groups, columns), 1) // states
        log_step = exactly(jnp.broadcast_to(step_ref[...], (8, all_groups)), head.astype(f32))[0:1]
        step_size = jnp.exp(log_step) / (rows * n_sp)
        exponent, angle = rate_real * step_size, rate_imag * step_size
        magnitude = jnp.exp(exponent)
        cosine = jnp.cos(angle)
        decay_real, decay_imag = magnitude * cosine, magnitude * jnp.sin(angle)
        series = jnp.ones_like(exponent)
        for k in range(10, 1, -1):
            series = 1.0 + series * exponent * (1.0 / k)
        growth = jnp.where(jnp.abs(exponent) < 0.5, exponent * series, magnitude - 1.0)
        less_one = growth * cosine - 2.0 * jnp.square(jnp.sin(0.5 * angle))
        denominator = rate_real * rate_real + rate_imag * rate_imag
        factors.append((less_one * rate_real + decay_imag * rate_imag) / denominator)
        factors.append((decay_imag * rate_real - less_one * rate_imag) / denominator)
        dec_ref[0:1, :] = decay_real
        dec_ref[1:2, :] = decay_imag

    def spread(k):
        high, low = split(matrices[k].reshape(width, states))
        return dot(high, tile_half) + dot(low, tile_half)

    def build_drive(i):
        same = iota((width, columns), 0) // SSM_GROUP == iota((width, columns), 1) // states
        real, imag = spread(0), spread(1)
        if i == 0:
            drive = factors[0] * real - factors[1] * imag
        else:
            drive = factors[0] * imag + factors[1] * real
        for j, piece in enumerate(split(jnp.where(same, drive, 0.0))):
            dmat[i, j] = piece

    def build_read(i):
        across = (iota((columns, states), 0) % states == iota((columns, states), 1)).astype(bf16)
        same = iota((columns, width), 0) // states == iota((columns, width), 1) // SSM_GROUP
        for j, piece in enumerate(split(matrices[2 + i].reshape(width, states))):
            rmat[i, j] = jnp.where(same, dot_nt(across, piece), 0.0).astype(bf16)

    def build_pool():
        across = (
            iota((POOL_GROUP, pool_width), 0) == iota((POOL_GROUP, pool_width), 1) % POOL_GROUP
        ).astype(bf16)
        same = iota((pool_width, pool_width), 0) // POOL_GROUP == iota((pool_width, pool_width), 1) // POOL_GROUP
        own = pool_own[...].reshape(pool_width, POOL_GROUP)
        pmat[...] = jnp.where(same, dot(own, across), 0.0).astype(bf16)

    squares = []

    def take(t):
        block = tok_full[t].astype(f32)
        squares.append(jnp.sum(block * block, axis=1, keepdims=True))
        cut = slice(t * features, (t + 1) * features)
        scaled[:, cut] = (block * gain_ref[:, cut]).astype(bf16)

    def tokens_in():
        owns[4].wait()
        for k in range(1, n_tp):
            pltpu.make_async_remote_copy(
                tok_ref, tok_full.at[(tp - k + n_tp) % n_tp], tok_send.at[k - 1], tok_recv.at[k - 1],
                device_id=(me, (tp + k) % n_tp), device_id_type=MESH,
            ).wait_recv()

    half = len(turns) // 2
    for work in (
        build_decay, lambda: build_drive(0), lambda: build_drive(1), lambda: build_read(0),
        lambda: build_read(1), build_pool,
    ):
        work()
        step(half)
    while turn[0] < half - n_tp:
        step(half)
    tokens_in()
    for t in range(n_tp):
        take(t)
        step(half)
    while turn[0] < half:
        step(half)
    owns[0].wait()
    owns[1].wait()
    inverse = lax.rsqrt(sum(squares) / (features * n_tp) + epsilon)
    state_in = (dot(scaled[...], wsi[...]) * inverse).astype(bf16)
    step()
    pool_in = (dot(scaled[...], wpi[...]) * inverse).astype(bf16)
    ext[window_reach:] = pool_in
    halo_out[...] = pool_in[rows - window_reach :]
    halo_copy = pltpu.make_async_remote_copy(
        halo_out, halo, halo_sem.at[0], halo_sem.at[1],
        device_id=((me + 1) % n_sp, tp), device_id_type=MESH,
    )
    step()
    shuffle = (
        iota((rows, rows), 1)
        == (iota((rows, rows), 0) % CHUNKS) * span + iota((rows, rows), 0) // CHUNKS
    ).astype(bf16)
    signal = dot(shuffle, state_in).astype(bf16)
    for i in range(2):
        push[i] = dot(signal, dmat[i, 0]) + dot(signal, dmat[i, 1])
        if i == 0:
            halo_copy.start()
        step()
    decay_real = jnp.broadcast_to(dec_ref[0:1, :], (CHUNKS, columns))
    decay_imag = jnp.broadcast_to(dec_ref[1:2, :], (CHUNKS, columns))

    def advance(p, carry):
        cut = pl.ds(pl.multiple_of(p * CHUNKS, CHUNKS), CHUNKS)
        real, imag = cmul(decay_real, decay_imag, *carry)
        real, imag = real + push[0, cut, :], imag + push[1, cut, :]
        push[0, cut, :] = real
        push[1, cut, :] = imag
        return real, imag

    zero = jnp.zeros((CHUNKS, columns), f32)
    end_real, end_imag = lax.fori_loop(0, span, advance, (zero, zero))

    def power(real, imag, count):
        out = None
        while count:
            if count % 2:
                out = (real, imag) if out is None else cmul(*out, real, imag)
            real, imag = cmul(real, imag, real, imag)
            count //= 2
        return out

    chunk_decay = power(dec_ref[0:1, :], dec_ref[1:2, :], span)
    block_decay = power(*chunk_decay, CHUNKS)
    row_zero = jnp.zeros((1, columns), f32)
    total = (row_zero, row_zero)
    for j in range(CHUNKS):
        moved = cmul(*chunk_decay, *total)
        total = (moved[0] + end_real[j : j + 1], moved[1] + end_imag[j : j + 1])
    which = iota((CHUNKS, columns), 0)
    ends[me] = jnp.where(which == 0, total[0], jnp.where(which == 1, total[1], 0.0))
    step()

    def end_copy(k):
        return pltpu.make_async_remote_copy(
            ends.at[me], ends.at[me], end_send.at[k - 1], end_recv.at[k - 1],
            device_id=((me + k) % n_sp, tp), device_id_type=MESH,
        )

    for k in range(1, n_sp):
        end_copy(k).start()

    halo_copy.wait_recv()
    ext[:window_reach] = jnp.where(me == 0, jnp.zeros_like(halo), halo[...])
    group = tp * (pool_width // POOL_GROUP) + iota((rows, pool_width), 1) // POOL_GROUP
    window = jnp.left_shift(jnp.ones_like(group), group % 4 + 1)
    targets = iota((rows, rows + window_reach), 0) + window_reach
    sources = iota((rows, rows + window_reach), 1)
    whole = ext[...]
    sums = jnp.zeros((rows, pool_width), f32)
    for power_index in range(1, 5):
        reach = 2**power_index
        band = ((sources <= targets) & (sources > targets - reach)).astype(bf16)
        sums = jnp.where(window == reach, dot(band, whole), sums)
        if power_index == 2:
            step()
    position = me * rows + iota((rows, pool_width), 0)
    divisor = jnp.minimum(position + 1, window).astype(f32)
    pooled = sums / divisor - ext[window_reach:].astype(f32)
    pooled_high, pooled_low = split(pooled)
    pool_gain = pg_ref[:, pl.ds(pl.multiple_of(tp * pool_width, pool_width), pool_width)]
    projected = dot(pooled_high, pmat[...]) + dot(pooled_low, pmat[...])
    mine_p[...] = (projected * pool_gain).astype(bf16)
    step()

    def act_copy(which, k, source):
        mine = mine_s if which == 0 else mine_p
        return pltpu.make_async_remote_copy(
            mine, act.at[which, source], act_send.at[which, k - 1], act_recv.at[which, k - 1],
            device_id=(me, (tp + k) % n_tp), device_id_type=MESH,
        )

    for k in range(1, n_tp):
        act_copy(1, k, tp).start()
    act[1, tp] = mine_p[...]

    step()
    for k in range(1, n_sp):
        there = ends.at[(me - k + n_sp) % n_sp]
        pltpu.make_async_remote_copy(
            there, there, end_send.at[k - 1], end_recv.at[k - 1],
            device_id=((me + k) % n_sp, tp), device_id_type=MESH,
        ).wait_recv()
    total = (row_zero, row_zero)
    for s in range(n_sp - 1):
        moved = cmul(*block_decay, *total)
        use = s < me
        total = (
            jnp.where(use, moved[0] + ends[s, 0:1, :], total[0]),
            jnp.where(use, moved[1] + ends[s, 1:2, :], total[1]),
        )
    begin_real, begin_imag = zero, zero
    for j in range(CHUNKS):
        begin_real = jnp.where(which == j, total[0], begin_real)
        begin_imag = jnp.where(which == j, total[1], begin_imag)
        moved = cmul(*chunk_decay, *total)
        total = (moved[0] + end_real[j : j + 1], moved[1] + end_imag[j : j + 1])

    def add_carry(p, carry):
        cut = pl.ds(pl.multiple_of(p * CHUNKS, CHUNKS), CHUNKS)
        real, imag = cmul(decay_real, decay_imag, *carry)
        push[0, cut, :] = push[0, cut, :] + real
        push[1, cut, :] = push[1, cut, :] + imag
        return real, imag

    lax.fori_loop(0, span, add_carry, (begin_real, begin_imag))
    step()
    step()
    real_high, real_low = split(push[0])
    imag_high, imag_low = split(push[1])
    readout = dot(real_high, rmat[0, 0]) + dot(real_high, rmat[0, 1]) + dot(real_low, rmat[0, 0])
    step()
    readout -= dot(imag_high, rmat[1, 0]) + dot(imag_high, rmat[1, 1]) + dot(imag_low, rmat[1, 0])
    skip = skip_ref[:, pl.ds(pl.multiple_of(tp * width, width), width)]
    readout += skip * signal.astype(f32)
    shuffled = jax.nn.gelu(readout).astype(bf16)
    restore = (
        iota((rows, rows), 0)
        == (iota((rows, rows), 1) % CHUNKS) * span + iota((rows, rows), 1) // CHUNKS
    ).astype(bf16)
    mine_s[...] = dot(restore, shuffled).astype(bf16)
    step()
    for k in range(1, n_tp):
        act_copy(0, k, tp).start()
    act[0, tp] = mine_s[...]
    while turn[0] < len(turns):
        step()
    for which in (1, 0):
        for k in range(1, n_tp):
            act_copy(which, k, (tp - k + n_tp) % n_tp).wait_recv()
    owns[2].wait()
    owns[3].wait()
    result = None
    for t in range(n_tp):
        for which, full, size in ((1, wpo, pool_width), (0, wso, width)):
            term = dot(act[which, t], full[t * size : (t + 1) * size, :])
            result = term if result is None else result + term
    out_ref[...] = result.astype(bf16)

    for a in range(4):
        for s in range(n_sp - 1):
            for h in range(PIECES):
                sender(a, s, h).wait_send()
    for k in range(1, n_tp):
        token_copy(k).wait_send()
        act_copy(0, k, tp).wait_send()
        act_copy(1, k, tp).wait_send()
    halo_copy.wait_send()
    for k in range(1, n_sp):
        end_copy(k).wait_send()


def body(
    n_sp, n_tp, n_x,
    tokens, norm_gain, state_in_weight, pool_in_weight, rate_real, rate_imag, log_step,
    input_real, input_imag, output_real, output_imag, skip_gain, pool_weight, pool_gain,
    state_out_weight, pool_out_weight,
):
    rows, features = tokens.shape
    in_rows, width = state_in_weight.shape
    pool_width = pool_in_weight.shape[1]
    out_rows, out_columns = state_out_weight.shape
    groups = width // SSM_GROUP
    states = rate_real.shape[1]
    columns = groups * states
    pool_groups = pool_width // POOL_GROUP
    vmem = pl.BlockSpec(memory_space=pltpu.VMEM)
    anywhere = pl.BlockSpec(memory_space=pl.ANY)
    dma = pltpu.SemaphoreType.DMA
    return pl.pallas_call(
        functools.partial(kernel, n_sp, n_tp, n_x, states),
        out_shape=jax.ShapeDtypeStruct((rows, out_columns), bf16),
        in_specs=[anywhere, vmem] + [anywhere] * 4 + [vmem] + [anywhere] * 4 + [vmem, anywhere, vmem]
        + [anywhere] * 2,
        out_specs=vmem,
        scratch_shapes=[
            pltpu.VMEM((n_tp, rows, features), bf16),
            pltpu.VMEM((n_sp * in_rows, width), bf16),
            pltpu.VMEM((n_sp * in_rows, pool_width), bf16),
            pltpu.VMEM((n_sp * out_rows, out_columns), bf16),
            pltpu.VMEM((n_sp * out_rows, out_columns), bf16),
            pltpu.VMEM((rows, features * n_tp), bf16),
            pltpu.VMEM((2, 2, width, columns), bf16),
            pltpu.VMEM((2, 2, columns, width), bf16),
            pltpu.VMEM((pool_width, pool_width), bf16),
            pltpu.VMEM((2, rows, columns), f32),
            pltpu.VMEM((rows + window_reach, pool_width), bf16),
            pltpu.VMEM((window_reach, pool_width), bf16),
            pltpu.VMEM((n_sp, CHUNKS, columns), f32),
            pltpu.VMEM((2, n_tp, rows, width), bf16),
            pltpu.VMEM((rows, width), bf16),
            pltpu.VMEM((rows, pool_width), bf16),
            pltpu.VMEM((window_reach, pool_width), bf16),
            pltpu.VMEM((2, groups, states), f32),
            pltpu.VMEM((4, groups, SSM_GROUP, states), f32),
            pltpu.VMEM((pool_groups, POOL_GROUP, POOL_GROUP), bf16),
            pltpu.VMEM((2, columns), f32),
            dma((12,)),
            dma((4, n_sp - 1, PIECES)),
            dma((4, n_sp - 1, PIECES)),
            dma((n_tp - 1,)),
            dma((n_tp - 1,)),
            dma((2, n_tp - 1)),
            dma((2, n_tp - 1)),
            dma((2,)),
            dma((n_sp - 1,)),
            dma((n_sp - 1,)),
        ],
        compiler_params=pltpu.CompilerParams(
            collective_id=0, has_side_effects=True, vmem_limit_bytes=60 * 2**20
        ),
    )(
        tokens, norm_gain[None], state_in_weight, pool_in_weight, rate_real, rate_imag, log_step[None],
        jnp.swapaxes(input_real, 1, 2), jnp.swapaxes(input_imag, 1, 2), output_real, output_imag,
        skip_gain[None], pool_weight, pool_gain[None], state_out_weight, pool_out_weight,
    )


def solution(mesh):
    n_sp, n_tp = mesh.shape["sp"], mesh.shape["tp"]
    n_x = 2 ** ((n_sp.bit_length() - 1) // 2)
    both, whole = P("sp", "tp"), P()
    return jax.shard_map(
        functools.partial(body, n_sp, n_tp, n_x),
        mesh=mesh,
        in_specs=(both, whole, both, both) + (whole,) * 10 + (both, both),
        out_specs=both,
        check_vma=False,
    )
```

```python
import functools

import jax
import jax.numpy as jnp
from jax import lax
from jax.experimental import pallas as pl
from jax.experimental.pallas import tpu as pltpu
from jax.sharding import PartitionSpec as P

SSM_GROUP = 16
POOL_GROUP = 64
CHUNKS = 8
PIECES = 2

epsilon = 1e-06
window_reach = 16
f32, bf16 = jnp.float32, jnp.bfloat16
MESH = pl.DeviceIdType.MESH


def discretize(rate_real, rate_imag, log_step, length):
    step_size = jnp.exp(log_step)[:, None] / length
    exponent = rate_real * step_size
    angle = rate_imag * step_size
    magnitude = jnp.exp(exponent)
    decay_real = magnitude * jnp.cos(angle)
    decay_imag = magnitude * jnp.sin(angle)
    less_one = jnp.expm1(exponent) * jnp.cos(angle) - 2.0 * jnp.square(jnp.sin(0.5 * angle))
    denominator = rate_real * rate_real + rate_imag * rate_imag
    factor_real = (less_one * rate_real + decay_imag * rate_imag) / denominator
    factor_imag = (decay_imag * rate_real - less_one * rate_imag) / denominator
    return decay_real, decay_imag, factor_real, factor_imag


def iota(shape, axis):
    return lax.broadcasted_iota(jnp.int32, shape, axis)


def dot(a, b):
    return jnp.dot(a, b, preferred_element_type=f32)


def dot_nt(a, b):
    return lax.dot_general(a, b, (((1,), (1,)), ((), ())), preferred_element_type=f32)


def split(a):
    high = a.astype(bf16)
    return high, (a - high.astype(f32)).astype(bf16)


def cmul(ar, ai, br, bi):
    return ar * br - ai * bi, ar * bi + ai * br


def kernel(
    n_sp, n_tp, n_x, states,
    tok_ref, gain_ref, wsi_ref, wpi_ref, rr_ref, ri_ref, step_ref, inr_ref, ini_ref, outr_ref,
    outi_ref, skip_ref, pw_ref, pg_ref, wso_ref, wpo_ref,
    out_ref,
    tok_full, wsi, wpi, wso, wpo, scaled, dmat, rmat, pmat, push, ext, halo, ends, act,
    mine_s, mine_p, halo_out, rates, matrices, pool_own, dec_ref,
    own_sem, ring_send, ring_recv, tok_send, tok_recv, act_send, act_recv, halo_sem, end_send, end_recv,
):
    me, tp = lax.axis_index("sp"), lax.axis_index("tp")
    n_z = n_sp // n_x
    rows = tok_ref.shape[0]
    features = tok_ref.shape[1]
    width = wsi_ref.shape[1]
    pool_width = wpi_ref.shape[1]
    groups = width // SSM_GROUP
    columns = groups * states
    pool_groups = pool_width // POOL_GROUP
    span = rows // CHUNKS

    def place(p):
        x, r = p // n_z, p % n_z
        return (r + (x % 2) * (n_z - 1 - 2 * r)) * n_x + x

    my_x, my_z = me % n_x, me // n_x
    at = my_x * n_z + my_z + (my_x % 2) * (n_z - 1 - 2 * my_z)

    barrier = pltpu.get_barrier_semaphore()
    for k in range(1, n_sp):
        pl.semaphore_signal(barrier, inc=1, device_id=((me + k) % n_sp, tp), device_id_type=MESH)
    for k in range(1, n_tp):
        pl.semaphore_signal(barrier, inc=1, device_id=(me, (tp + k) % n_tp), device_id_type=MESH)

    fulls = ((wsi_ref, wsi), (wpi_ref, wpi), (wso_ref, wso), (wpo_ref, wpo))
    owns = []
    for a, (own, full) in enumerate(fulls):
        count = own.shape[0]
        owns.append(
            pltpu.make_async_copy(
                own, full.at[pl.ds(pl.multiple_of(me * count, count), count)], own_sem.at[a]
            )
        )
    owns.append(pltpu.make_async_copy(tok_ref, tok_full.at[tp], own_sem.at[4]))
    def heads(ref, count):
        return ref.at[pl.ds(pl.multiple_of(tp * count, count), count)]

    loads = [
        pltpu.make_async_copy(heads(ref, groups), there, own_sem.at[5 + k])
        for k, (ref, there) in enumerate(
            (
                (rr_ref, rates.at[0]), (ri_ref, rates.at[1]), (inr_ref, matrices.at[0]),
                (ini_ref, matrices.at[1]), (outr_ref, matrices.at[2]), (outi_ref, matrices.at[3]),
            )
        )
    ]
    loads.append(pltpu.make_async_copy(heads(pw_ref, pool_groups), pool_own, own_sem.at[11]))
    for c in owns + loads:
        c.start()
    pl.semaphore_wait(barrier, n_sp - 1 + n_tp - 1)

    ways = (1, -1)

    def reach_of(a, d):
        return n_sp // 2 if a % 2 == d else n_sp - 1 - n_sp // 2

    def part(a, d, s, h):
        own, full = fulls[a]
        count = own.shape[0]
        size = count // PIECES
        way = ways[d]
        owner = place((at - way * s + n_sp) % n_sp)
        there = full.at[pl.ds(pl.multiple_of(owner * count + h * size, size), size)]
        source = own.at[pl.ds(h * size, size)] if s == 0 else there
        return source, there, (place((at + way + n_sp) % n_sp), tp)

    def sender(a, d, s, h):
        source, there, target = part(a, d, s, h)
        return pltpu.make_async_remote_copy(
            source, there, ring_send.at[a, d, s, h], ring_recv.at[a, d, s, h],
            device_id=target, device_id_type=MESH,
        )

    def arrive(a, d, s, h):
        _, there, target = part(a, d, s + 1, h)
        pltpu.make_async_remote_copy(
            there, there, ring_send.at[a, d, s, h], ring_recv.at[a, d, s, h],
            device_id=target, device_id_type=MESH,
        ).wait_recv()

    longest = n_sp // 2

    def ring(phase, s, h):
        streams = [
            (a, d) for a in (2 * phase, 2 * phase + 1) for d in range(2) if s < reach_of(a, d)
        ]
        for a, d in sorted(streams, key=lambda i: -reach_of(*i)):
            arrive(a, d, s, h)
            if s + 1 < reach_of(a, d):
                sender(a, d, s + 1, h).start()
        if phase == 0 and h == PIECES - 1:
            for a, d in streams:
                if s + 1 == reach_of(a, d):
                    for g in range(PIECES):
                        sender(a + 2, d, 0, g).start()

    turns = [(phase, s, h) for phase in range(2) for s in range(longest) for h in range(PIECES)]
    turn = [0]

    def step(stop=len(turns)):
        if turn[0] < stop:
            ring(*turns[turn[0]])
            turn[0] += 1

    def token_copy(k):
        return pltpu.make_async_remote_copy(
            tok_ref, tok_full.at[tp], tok_send.at[k - 1], tok_recv.at[k - 1],
            device_id=(me, (tp + k) % n_tp), device_id_type=MESH,
        )

    for h in range(PIECES):
        for a, d in ((0, 0), (1, 1), (0, 1), (1, 0)):
            sender(a, d, 0, h).start()
    for k in range(1, n_tp):
        token_copy(k).start()

    tile = iota((states, columns), 0) == iota((states, columns), 1) % states
    tile_exact, tile_half = tile.astype(f32), tile.astype(bf16)

    def exactly(a, b):
        return jnp.dot(a, b, precision=lax.Precision.HIGHEST, preferred_element_type=f32)

    factors = []

    def build_decay():
        for c in loads:
            c.wait()
        own_head = iota((groups, columns), 0) == iota((groups, columns), 1) // states

        def flat(a):
            return jnp.sum(jnp.where(own_head, exactly(a, tile_exact), 0.0), axis=0, keepdims=True)

        rate_real, rate_imag = flat(rates[0]), flat(rates[1])
        all_groups = step_ref.shape[1]
        head = iota((all_groups, columns), 0) == tp * groups + iota((all_groups, columns), 1) // states
        log_step = exactly(jnp.broadcast_to(step_ref[...], (8, all_groups)), head.astype(f32))[0:1]
        step_size = jnp.exp(log_step) / (rows * n_sp)
        exponent, angle = rate_real * step_size, rate_imag * step_size
        magnitude = jnp.exp(exponent)
        cosine = jnp.cos(angle)
        decay_real, decay_imag = magnitude * cosine, magnitude * jnp.sin(angle)
        series = jnp.ones_like(exponent)
        for k in range(10, 1, -1):
            series = 1.0 + series * exponent * (1.0 / k)
        growth = jnp.where(jnp.abs(exponent) < 0.5, exponent * series, magnitude - 1.0)
        less_one = growth * cosine - 2.0 * jnp.square(jnp.sin(0.5 * angle))
        denominator = rate_real * rate_real + rate_imag * rate_imag
        factors.append((less_one * rate_real + decay_imag * rate_imag) / denominator)
        factors.append((decay_imag * rate_real - less_one * rate_imag) / denominator)
        dec_ref[0:1, :] = decay_real
        dec_ref[1:2, :] = decay_imag

    def spread(k):
        high, low = split(matrices[k].reshape(width, states))
        return dot(high, tile_half) + dot(low, tile_half)

    def build_drive(i):
        same = iota((width, columns), 0) // SSM_GROUP == iota((width, columns), 1) // states
        real, imag = spread(0), spread(1)
        if i == 0:
            drive = factors[0] * real - factors[1] * imag
        else:
            drive = factors[0] * imag + factors[1] * real
        for j, piece in enumerate(split(jnp.where(same, drive, 0.0))):
            dmat[i, j] = piece

    def build_read(i):
        across = (iota((columns, states), 0) % states == iota((columns, states), 1)).astype(bf16)
        same = iota((columns, width), 0) // states == iota((columns, width), 1) // SSM_GROUP
        for j, piece in enumerate(split(matrices[2 + i].reshape(width, states))):
            rmat[i, j] = jnp.where(same, dot_nt(across, piece), 0.0).astype(bf16)

    def build_pool():
        across = (
            iota((POOL_GROUP, pool_width), 0) == iota((POOL_GROUP, pool_width), 1) % POOL_GROUP
        ).astype(bf16)
        same = iota((pool_width, pool_width), 0) // POOL_GROUP == iota((pool_width, pool_width), 1) // POOL_GROUP
        own = pool_own[...].reshape(pool_width, POOL_GROUP)
        pmat[...] = jnp.where(same, dot(own, across), 0.0).astype(bf16)

    squares = []

    def take(t):
        block = tok_full[t].astype(f32)
        squares.append(jnp.sum(block * block, axis=1, keepdims=True))
        cut = slice(t * features, (t + 1) * features)
        scaled[:, cut] = (block * gain_ref[:, cut]).astype(bf16)

    def tokens_in():
        owns[4].wait()
        for k in range(1, n_tp):
            pltpu.make_async_remote_copy(
                tok_ref, tok_full.at[(tp - k + n_tp) % n_tp], tok_send.at[k - 1], tok_recv.at[k - 1],
                device_id=(me, (tp + k) % n_tp), device_id_type=MESH,
            ).wait_recv()

    half = len(turns) // 2
    for at_work, work in enumerate(
        (
            build_decay, lambda: build_drive(0), lambda: build_drive(1), lambda: build_read(0),
            lambda: build_read(1), build_pool,
        )
    ):
        work()
        if at_work in (0, 1, 3, 5):
            step(half)
    while turn[0] < half - 3:
        step(half)
    tokens_in()
    for t in range(n_tp):
        take(t)
        if t == n_tp // 2 - 1:
            step(half)
    while turn[0] < half:
        step(half)
    owns[0].wait()
    owns[1].wait()
    inverse = lax.rsqrt(sum(squares) / (features * n_tp) + epsilon)
    state_in = (dot(scaled[...], wsi[...]) * inverse).astype(bf16)
    pool_in = (dot(scaled[...], wpi[...]) * inverse).astype(bf16)
    ext[window_reach:] = pool_in
    halo_out[...] = pool_in[rows - window_reach :]
    halo_copy = pltpu.make_async_remote_copy(
        halo_out, halo, halo_sem.at[0], halo_sem.at[1],
        device_id=((me + 1) % n_sp, tp), device_id_type=MESH,
    )
    shuffle = (
        iota((rows, rows), 1)
        == (iota((rows, rows), 0) % CHUNKS) * span + iota((rows, rows), 0) // CHUNKS
    ).astype(bf16)
    signal = dot(shuffle, state_in).astype(bf16)
    for i in range(2):
        push[i] = dot(signal, dmat[i, 0]) + dot(signal, dmat[i, 1])
        if i == 0:
            halo_copy.start()
        else:
            step()
    decay_real = jnp.broadcast_to(dec_ref[0:1, :], (CHUNKS, columns))
    decay_imag = jnp.broadcast_to(dec_ref[1:2, :], (CHUNKS, columns))

    def advance(p, carry):
        cut = pl.ds(pl.multiple_of(p * CHUNKS, CHUNKS), CHUNKS)
        real, imag = cmul(decay_real, decay_imag, *carry)
        real, imag = real + push[0, cut, :], imag + push[1, cut, :]
        push[0, cut, :] = real
        push[1, cut, :] = imag
        return real, imag

    zero = jnp.zeros((CHUNKS, columns), f32)
    end_real, end_imag = lax.fori_loop(0, span, advance, (zero, zero))

    def power(real, imag, count):
        out = None
        while count:
            if count % 2:
                out = (real, imag) if out is None else cmul(*out, real, imag)
            real, imag = cmul(real, imag, real, imag)
            count //= 2
        return out

    chunk_decay = power(dec_ref[0:1, :], dec_ref[1:2, :], span)
    block_decay = power(*chunk_decay, CHUNKS)
    row_zero = jnp.zeros((1, columns), f32)
    total = (row_zero, row_zero)
    for j in range(CHUNKS):
        moved = cmul(*chunk_decay, *total)
        total = (moved[0] + end_real[j : j + 1], moved[1] + end_imag[j : j + 1])
    which = iota((CHUNKS, columns), 0)
    ends[me] = jnp.where(which == 0, total[0], jnp.where(which == 1, total[1], 0.0))

    def end_copy(k):
        return pltpu.make_async_remote_copy(
            ends.at[me], ends.at[me], end_send.at[k - 1], end_recv.at[k - 1],
            device_id=((me + k) % n_sp, tp), device_id_type=MESH,
        )

    for k in range(1, n_sp):
        end_copy(k).start()

    halo_copy.wait_recv()
    ext[:window_reach] = jnp.where(me == 0, jnp.zeros_like(halo), halo[...])
    group = tp * (pool_width // POOL_GROUP) + iota((rows, pool_width), 1) // POOL_GROUP
    window = jnp.left_shift(jnp.ones_like(group), group % 4 + 1)
    targets = iota((rows, rows + window_reach), 0) + window_reach
    sources = iota((rows, rows + window_reach), 1)
    whole = ext[...]
    sums = jnp.zeros((rows, pool_width), f32)
    for power_index in range(1, 5):
        reach = 2**power_index
        band = ((sources <= targets) & (sources > targets - reach)).astype(bf16)
        sums = jnp.where(window == reach, dot(band, whole), sums)
        if power_index == 2:
            step()
    position = me * rows + iota((rows, pool_width), 0)
    divisor = jnp.minimum(position + 1, window).astype(f32)
    pooled = sums / divisor - ext[window_reach:].astype(f32)
    pooled_high, pooled_low = split(pooled)
    pool_gain = pg_ref[:, pl.ds(pl.multiple_of(tp * pool_width, pool_width), pool_width)]
    projected = dot(pooled_high, pmat[...]) + dot(pooled_low, pmat[...])
    mine_p[...] = (projected * pool_gain).astype(bf16)
    step()

    def act_copy(which, k, source):
        mine = mine_s if which == 0 else mine_p
        return pltpu.make_async_remote_copy(
            mine, act.at[which, source], act_send.at[which, k - 1], act_recv.at[which, k - 1],
            device_id=(me, (tp + k) % n_tp), device_id_type=MESH,
        )

    for k in range(1, n_tp):
        act_copy(1, k, tp).start()
    act[1, tp] = mine_p[...]

    for k in range(1, n_sp):
        there = ends.at[(me - k + n_sp) % n_sp]
        pltpu.make_async_remote_copy(
            there, there, end_send.at[k - 1], end_recv.at[k - 1],
            device_id=((me + k) % n_sp, tp), device_id_type=MESH,
        ).wait_recv()
    total = (row_zero, row_zero)
    for s in range(n_sp - 1):
        moved = cmul(*block_decay, *total)
        use = s < me
        total = (
            jnp.where(use, moved[0] + ends[s, 0:1, :], total[0]),
            jnp.where(use, moved[1] + ends[s, 1:2, :], total[1]),
        )
    begin_real, begin_imag = zero, zero
    for j in range(CHUNKS):
        begin_real = jnp.where(which == j, total[0], begin_real)
        begin_imag = jnp.where(which == j, total[1], begin_imag)
        moved = cmul(*chunk_decay, *total)
        total = (moved[0] + end_real[j : j + 1], moved[1] + end_imag[j : j + 1])

    def add_carry(p, carry):
        cut = pl.ds(pl.multiple_of(p * CHUNKS, CHUNKS), CHUNKS)
        real, imag = cmul(decay_real, decay_imag, *carry)
        push[0, cut, :] = push[0, cut, :] + real
        push[1, cut, :] = push[1, cut, :] + imag
        return real, imag

    lax.fori_loop(0, span, add_carry, (begin_real, begin_imag))
    step()
    real_high, real_low = split(push[0])
    imag_high, imag_low = split(push[1])
    readout = dot(real_high, rmat[0, 0]) + dot(real_high, rmat[0, 1]) + dot(real_low, rmat[0, 0])
    step()
    readout -= dot(imag_high, rmat[1, 0]) + dot(imag_high, rmat[1, 1]) + dot(imag_low, rmat[1, 0])
    skip = skip_ref[:, pl.ds(pl.multiple_of(tp * width, width), width)]
    readout += skip * signal.astype(f32)
    shuffled = jax.nn.gelu(readout).astype(bf16)
    restore = (
        iota((rows, rows), 0)
        == (iota((rows, rows), 1) % CHUNKS) * span + iota((rows, rows), 1) // CHUNKS
    ).astype(bf16)
    mine_s[...] = dot(restore, shuffled).astype(bf16)
    for k in range(1, n_tp):
        act_copy(0, k, tp).start()
    act[0, tp] = mine_s[...]
    while turn[0] < len(turns):
        step()
    for which in (1, 0):
        for k in range(1, n_tp):
            act_copy(which, k, (tp - k + n_tp) % n_tp).wait_recv()
    owns[2].wait()
    owns[3].wait()
    result = None
    for t in range(n_tp):
        for which, full, size in ((1, wpo, pool_width), (0, wso, width)):
            term = dot(act[which, t], full[t * size : (t + 1) * size, :])
            result = term if result is None else result + term
    out_ref[...] = result.astype(bf16)

    for a in range(4):
        for d in range(2):
            for s in range(reach_of(a, d)):
                for h in range(PIECES):
                    sender(a, d, s, h).wait_send()
    for k in range(1, n_tp):
        token_copy(k).wait_send()
        act_copy(0, k, tp).wait_send()
        act_copy(1, k, tp).wait_send()
    halo_copy.wait_send()
    for k in range(1, n_sp):
        end_copy(k).wait_send()


def body(
    n_sp, n_tp, n_x,
    tokens, norm_gain, state_in_weight, pool_in_weight, rate_real, rate_imag, log_step,
    input_real, input_imag, output_real, output_imag, skip_gain, pool_weight, pool_gain,
    state_out_weight, pool_out_weight,
):
    rows, features = tokens.shape
    in_rows, width = state_in_weight.shape
    pool_width = pool_in_weight.shape[1]
    out_rows, out_columns = state_out_weight.shape
    groups = width // SSM_GROUP
    states = rate_real.shape[1]
    columns = groups * states
    pool_groups = pool_width // POOL_GROUP
    vmem = pl.BlockSpec(memory_space=pltpu.VMEM)
    anywhere = pl.BlockSpec(memory_space=pl.ANY)
    dma = pltpu.SemaphoreType.DMA
    return pl.pallas_call(
        functools.partial(kernel, n_sp, n_tp, n_x, states),
        out_shape=jax.ShapeDtypeStruct((rows, out_columns), bf16),
        in_specs=[anywhere, vmem] + [anywhere] * 4 + [vmem] + [anywhere] * 4 + [vmem, anywhere, vmem]
        + [anywhere] * 2,
        out_specs=vmem,
        scratch_shapes=[
            pltpu.VMEM((n_tp, rows, features), bf16),
            pltpu.VMEM((n_sp * in_rows, width), bf16),
            pltpu.VMEM((n_sp * in_rows, pool_width), bf16),
            pltpu.VMEM((n_sp * out_rows, out_columns), bf16),
            pltpu.VMEM((n_sp * out_rows, out_columns), bf16),
            pltpu.VMEM((rows, features * n_tp), bf16),
            pltpu.VMEM((2, 2, width, columns), bf16),
            pltpu.VMEM((2, 2, columns, width), bf16),
            pltpu.VMEM((pool_width, pool_width), bf16),
            pltpu.VMEM((2, rows, columns), f32),
            pltpu.VMEM((rows + window_reach, pool_width), bf16),
            pltpu.VMEM((window_reach, pool_width), bf16),
            pltpu.VMEM((n_sp, CHUNKS, columns), f32),
            pltpu.VMEM((2, n_tp, rows, width), bf16),
            pltpu.VMEM((rows, width), bf16),
            pltpu.VMEM((rows, pool_width), bf16),
            pltpu.VMEM((window_reach, pool_width), bf16),
            pltpu.VMEM((2, groups, states), f32),
            pltpu.VMEM((4, groups, SSM_GROUP, states), f32),
            pltpu.VMEM((pool_groups, POOL_GROUP, POOL_GROUP), bf16),
            pltpu.VMEM((2, columns), f32),
            dma((12,)),
            dma((4, 2, n_sp // 2, PIECES)),
            dma((4, 2, n_sp // 2, PIECES)),
            dma((n_tp - 1,)),
            dma((n_tp - 1,)),
            dma((2, n_tp - 1)),
            dma((2, n_tp - 1)),
            dma((2,)),
            dma((n_sp - 1,)),
            dma((n_sp - 1,)),
        ],
        compiler_params=pltpu.CompilerParams(
            collective_id=0, has_side_effects=True, vmem_limit_bytes=60 * 2**20
        ),
    )(
        tokens, norm_gain[None], state_in_weight, pool_in_weight, rate_real, rate_imag, log_step[None],
        jnp.swapaxes(input_real, 1, 2), jnp.swapaxes(input_imag, 1, 2), output_real, output_imag,
        skip_gain[None], pool_weight, pool_gain[None], state_out_weight, pool_out_weight,
    )


def solution(mesh):
    n_sp, n_tp = mesh.shape["sp"], mesh.shape["tp"]
    n_x = 2 ** ((n_sp.bit_length() - 1) // 2)
    both, whole = P("sp", "tp"), P()
    return jax.shard_map(
        functools.partial(body, n_sp, n_tp, n_x),
        mesh=mesh,
        in_specs=(both, whole, both, both) + (whole,) * 10 + (both, both),
        out_specs=both,
        check_vma=False,
    )
```
